256 devices in a mesh: grp: 2 (over y), sp: 32 (over z, core), tp: 4 (over x).
Axes of the slice: x: 4, y: 2, z: 16, core: 2. Of those that a mesh axis runs over, the one named last changes fastest.
The devices are a block of a 4x16x16 slice.
Arguments:
- gate_in: bfloat16 [32768, 1536], P(('grp', 'sp'), 'tp'), parts along dimension 0, may hold values from -6 to 6
- mult_in: bfloat16 [32768, 1536], P(('grp', 'sp'), 'tp'), parts along dimension 0, may hold values from -6 to 6
- value_in: bfloat16 [32768, 1536], P(('grp', 'sp'), 'tp'), parts along dimension 0, may hold values from -6 to 6
- doc_ids: int32 [32768], P(('grp', 'sp')), parts along dimension 0, may hold values from 0 to 15, never falling along the last dimension, each value on 1 to 1536 neighbouring positions
- conv_taps: bfloat16 [3, 1536], P(None, 'tp'), may hold values from -3 to 3
- out_proj: bfloat16 [1536, 2048], P('tp'), may hold values from -0.15625 to 0.15625
- resid: bfloat16 [32768, 2048], P(('grp', 'sp', 'tp')), parts along dimension 0, may hold values from -6 to 6
- norm1_gain: float32 [2048], replicated, may hold values from 0.1 to 1.9
- norm1_bias: float32 [2048], replicated, may hold values from -1.5 to 1.5
- expert_ids: int32 [32768, 2], P(('grp', 'sp', 'tp')), parts along dimension 0, may hold values from 0 to 31, all different within a row; in each aligned block of 128 rows (0 to 127, 128 to 255, ...) at most 10 rows name the same one
- expert_wts: float32 [32768, 2], P(('grp', 'sp', 'tp')), parts along dimension 0, may hold values from 0.1 to 1
- w_gate: bfloat16 [32, 2048, 3072], P('sp', None, 'tp'), may hold values from -0.125 to 0.125
- w_up: bfloat16 [32, 2048, 3072], P('sp', None, 'tp'), may hold values from -0.125 to 0.125
- w_down: bfloat16 [32, 3072, 2048], P('sp', 'tp'), may hold values from -0.21582031 to 0.21582031
- norm2_gain: float32 [2048], replicated, may hold values from 0.1 to 1.9
- norm2_bias: float32 [2048], replicated, may hold values from -1.5 to 1.5
Outputs:
- result: bfloat16 [32768, 2048], P(('grp', 'sp', 'tp')), parts along dimension 0
The draws below stay inside these ranges and needn't reach their ends.
There are 2 independent parts, one for each index of `grp`. The reference program is written for one: setup_inputs(seed, part) draws one part's arguments, and reference() takes and returns one part's arrays. A program takes and returns all parts, laid end to end along the dimension named above; an argument that names none is the same for every part. Nothing has to cross between parts.
Inputs may be any that keep to these rules, and one draw needn't show every extreme that they name: `doc_ids`: never falling along the sequence; each document has 1 to 1536 positions and one has exactly 1536. `expert_ids`: each row names 2 different experts. Among the rows of one device no expert is named more than 10 times, and in some device's rows some expert is named exactly 10 times.
All inputs are finite; a program needn't handle non-finite values.
Results may differ from the reference program's by a relative error of at most 0.0095.
Values may be sent and summed in bfloat16 or wider, within the bound.
No kernel may reach another device: no remote copies, remote signals or barrier semaphores. Data moves between devices by JAX's collectives and lax.ppermute only.
A program may use at most 128 MiB of HBM per device.

```python
import math
import jax
import jax.numpy as jnp
import numpy as np
from jax import lax

D = 2048
D_CONV = 1536
FF_E = 3072
KW = 3
TOPK = 2
TOK_DEV = 128
TOKENS = 16384
EXPERTS = 32
CAP = 10
DOCS = 16
DOC_MOST = 1536
N_TP = 4


def block_levels(rng, extent, shards, smallest, largest):
    loudness, own = 1.0, jax.random.fold_in(rng, 6)
    for dim, shards_of in shards:
        steps = jnp.exp(jax.random.uniform(jax.random.fold_in(own, dim), (shards_of,), jnp.float32, smallest / len(shards), largest / len(shards)))
        loudness = loudness * jnp.repeat(steps, extent[dim] // shards_of).reshape([-1 if axis == dim else 1 for axis in range(len(extent))])
    return loudness


def profile(number_of, total, reach, skew):
    weights = [(1 << 20) // math.isqrt(grade ** skew) + 1 for grade in range(2, number_of + 1)]
    surplus, counts = total - reach - (number_of - 1), [1] * (number_of - 1)
    while surplus > 0:
        candidates = [i for i in range(number_of - 1) if counts[i] < reach]
        whole, left = sum([weights[i] for i in candidates]), surplus
        for i in candidates:
            extra = min(reach - counts[i], max(1, left * weights[i] // whole), surplus)
            counts[i] = counts[i] + extra
            surplus = surplus - extra
    return np.array([reach] + counts)


def ragged_sizes(rng, number_of, total, limit, lean):
    if number_of == 2:
        one = jax.random.randint(rng, (), max(1, total - limit), min(limit, total - 1) + 1)
        return jnp.stack([one, total - one])
    tallies = jnp.asarray(profile(number_of, total, limit, lean), jnp.int32)
    twos = (number_of - 1) // 2
    donor, receiver = tallies[1:1 + 2 * twos:2], tallies[2:2 + 2 * twos:2]
    room = jnp.minimum(donor - 1, limit - receiver)
    moved = jax.random.randint(jax.random.fold_in(rng, 1), (twos,), 0, 1 << 20) % (room + 1)
    tallies = tallies.at[1:1 + 2 * twos:2].set(donor - moved).at[2:2 + 2 * twos:2].set(receiver + moved)
    return tallies[jax.random.permutation(jax.random.fold_in(rng, 2), number_of)]


def routed_block(key, own, number, rows, number_of, top, most, lean):
    ranking = jax.random.permutation(key, number_of)
    packed, ordinary = shares(number_of, rows * top, most, lean, True), shares(number_of, rows * top, most, lean, False)
    places = jnp.arange(number_of)

    def named(lengths, offset_by):
        used = int((lengths > 0).sum())
        fixed = max(1, used // 4)
        passed = fixed + (places - fixed + offset_by * (used - fixed)) % max(1, number_of - fixed)
        return jnp.zeros((number_of,), jnp.int32).at[ranking[jnp.where(places < fixed, places, passed)]].set(jnp.asarray(lengths, jnp.int32))

    lengths = jnp.where(number % 4 == 0, named(packed, number // 4), named(ordinary, number - number // 4 - 1))
    mixed = jax.random.permutation(jax.random.fold_in(own, 3), number_of)
    donor, receiver = mixed[0:number_of // 2 * 2:2], mixed[1:number_of // 2 * 2:2]
    slack = jnp.minimum(lengths[donor] - 1, most - lengths[receiver]) // 2
    slack = jnp.where((donor == ranking[0]) | (receiver == ranking[0]) | (lengths[receiver] == 0), 0, jnp.maximum(slack, 0))
    passed = jax.random.randint(jax.random.fold_in(own, 4), (number_of // 2,), 0, 1 << 20) % (slack + 1)
    lengths = lengths.at[donor].add(-passed).at[receiver].add(passed)
    items = jnp.searchsorted(jnp.cumsum(lengths), jnp.arange(rows * top), side="right").astype(jnp.int32)
    table = items.reshape(top, rows).T
    table = table[jax.random.permutation(jax.random.fold_in(own, 1), rows)]
    offset_by = jax.random.randint(jax.random.fold_in(own, 2), (rows, 1), 0, top)
    return jnp.take_along_axis(table, (jnp.arange(top)[None, :] + offset_by) % top, axis=1)


def shares(number_of, total, limit, skew, full):
    portions = [(1 << 20) // math.isqrt(grade ** skew) + 1 for grade in range(1, number_of + 1)]
    largest = limit if full else min(limit, max(-(-total // number_of), total * portions[0] // sum(portions)))
    least = 1 if total - largest >= number_of - 1 else 0
    counts, surplus = [largest] + [least] * (number_of - 1), total - largest - least * (number_of - 1)
    while surplus > 0:
        candidates = [i for i in range(1, number_of) if counts[i] < largest] or [i for i in range(1, number_of) if counts[i] < limit]
        whole, left = sum([portions[i] for i in candidates]), surplus
        for i in candidates:
            more = min(limit - counts[i], max(1, left * portions[i] // whole), surplus)
            counts[i] = counts[i] + more
            surplus = surplus - more
    return np.array(counts)


def scatter_about(own_key, extent, width, most, split=(), kind=jnp.bfloat16):
    result = jax.random.normal(own_key, extent, jnp.float32) * width
    if len(split) > 0:
        result = block_levels(own_key, extent, split, -0.22, 0.18) * result
    return jnp.clip(result, min=-most, max=most).astype(kind)


def setup_inputs(seed: int = 0, part: int = 0) -> dict:
    streams_of = jax.random.split(jax.random.key(seed), 17)
    part_keys = jax.random.split(jax.random.fold_in(streams_of[16], part), 17)
    gate_in = scatter_about(part_keys[0], (TOKENS, D_CONV), 1.0, 6.0, ((0, 32), (1, 4)))
    mult_in = scatter_about(part_keys[1], (TOKENS, D_CONV), 1.0, 6.0, ((0, 32), (1, 4)))
    value_in = scatter_about(part_keys[2], (TOKENS, D_CONV), 1.0, 6.0, ((0, 32), (1, 4)))
    doc_ids = jnp.searchsorted(jnp.cumsum(ragged_sizes(part_keys[3], DOCS, TOKENS, DOC_MOST, 1)), jnp.arange(TOKENS), side="right").astype(jnp.int32)
    conv_taps = scatter_about(streams_of[4], (KW, D_CONV), 0.577, 3.0, ((1, 4),))
    out_proj = scatter_about(streams_of[5], (D_CONV, D), D_CONV ** -0.5, 0.15625, ((0, 4),))
    resid = scatter_about(part_keys[6], (TOKENS, D), 1.0, 6.0, ((0, 128),))
    norm1_gain = jnp.clip(1.0 + 0.18 * jax.random.normal(streams_of[7], (D,), jnp.float32), 0.1, 1.9)
    norm1_bias = scatter_about(streams_of[8], (D,), 0.3, 1.5, (), jnp.float32)
    expert_ids_keys = jax.random.split(jax.random.fold_in(part_keys[9], 1), TOKENS // TOK_DEV)
    expert_ids_turns = jax.random.permutation(jax.random.fold_in(part_keys[9], 3), TOKENS // TOK_DEV)
    expert_ids = jax.vmap(lambda own, number: routed_block(jax.random.fold_in(part_keys[9], 2), own, number, TOK_DEV, EXPERTS, TOPK, CAP, 2))(expert_ids_keys, expert_ids_turns).reshape((TOKENS, TOPK))
    expert_wts = jnp.clip(0.1 + 0.9 * jax.random.uniform(part_keys[10], (TOKENS, TOPK), jnp.float32) ** block_levels(part_keys[10], (TOKENS, TOPK), ((0, 128),), -0.2, 0.2), 0.1, 1.0)
    w_gate = scatter_about(streams_of[11], (EXPERTS, D, FF_E), D ** -0.5, 0.125, ((0, 32), (2, 4)))
    w_up = scatter_about(streams_of[12], (EXPERTS, D, FF_E), D ** -0.5, 0.125, ((0, 32), (2, 4)))
    w_down = scatter_about(streams_of[13], (EXPERTS, FF_E, D), (2.0 / FF_E ** 0.5), 0.21582031, ((0, 32), (1, 4)))
    norm2_gain = jnp.clip(1.0 + 0.18 * jax.random.normal(streams_of[14], (D,), jnp.float32), 0.1, 1.9)
    norm2_bias = scatter_about(streams_of[15], (D,), 0.3, 1.5, (), jnp.float32)
    return dict(gate_in=gate_in, mult_in=mult_in, value_in=value_in, doc_ids=doc_ids, conv_taps=conv_taps, out_proj=out_proj, resid=resid, norm1_gain=norm1_gain, norm1_bias=norm1_bias, expert_ids=expert_ids, expert_wts=expert_wts, w_gate=w_gate, w_up=w_up, w_down=w_down, norm2_gain=norm2_gain, norm2_bias=norm2_bias)


residual_scale = 2.0 ** 0.5
norm_eps = 1e-05

def layer_norm(pre, gain, bias):
    center = pre - lax.optimization_barrier(jnp.mean(pre, axis=-1, keepdims=True))
    spread = lax.optimization_barrier(jnp.mean(center * center, axis=-1, keepdims=True))
    return center * lax.rsqrt(spread + norm_eps) * gain + bias

def reference(gate_in, mult_in, value_in, doc_ids, conv_taps, out_proj, resid, norm1_gain, norm1_bias, expert_ids, expert_wts, w_gate, w_up, w_down, norm2_gain, norm2_bias):
    tap_weights = conv_taps.astype(jnp.float32)
    product = mult_in.astype(jnp.float32) * value_in.astype(jnp.float32)
    row_count = product.shape[0]
    padded = jnp.pad(product, ((KW - 1, 0), (0, 0)))
    doc_padded = jnp.concatenate([jnp.full((KW - 1,), -1, jnp.int32), doc_ids.astype(jnp.int32)])
    filtered = jnp.zeros_like(product)
    for tap_index in range(KW):
        shifted = padded[tap_index:tap_index + row_count]
        same_doc = (doc_padded[tap_index:tap_index + row_count] == doc_ids)[:, None]
        filtered = filtered + tap_weights[tap_index] * jnp.where(same_doc, shifted, 0.0)
    mixed_heads = (gate_in.astype(jnp.float32) * filtered).astype(jnp.bfloat16)
    mixed = jnp.dot(mixed_heads, out_proj, preferred_element_type=jnp.float32)
    hidden_one = layer_norm(residual_scale * resid.astype(jnp.float32) + mixed, norm1_gain, norm1_bias).astype(jnp.bfloat16)
    flat_ids = expert_ids.reshape(-1)
    flat_wts = expert_wts.reshape(-1)
    most_rows = CAP * (TOKENS // TOK_DEV)
    part_width = FF_E // N_TP

    def one_expert(moe, inputs):
        gate_w, up_w, down_w, number = inputs
        chosen = flat_ids == number
        picks = jnp.nonzero(chosen, size=most_rows, fill_value=0)[0].astype(jnp.int32)
        live = jnp.arange(most_rows, dtype=jnp.int32) < jnp.sum(chosen.astype(jnp.int32))
        rows = (picks // TOPK).astype(jnp.int32)
        inputs_rows = hidden_one[rows]
        gate_act = jnp.dot(inputs_rows, gate_w, preferred_element_type=jnp.float32)
        up_act = jnp.dot(inputs_rows, up_w, preferred_element_type=jnp.float32)
        hid = (jax.nn.silu(gate_act) * up_act).astype(jnp.bfloat16)
        total = jnp.zeros((most_rows, D), jnp.float32)
        for part in range(N_TP):
            piece = jnp.dot(hid[:, part * part_width:(part + 1) * part_width], down_w[part * part_width:(part + 1) * part_width], preferred_element_type=jnp.float32).astype(jnp.bfloat16)
            total = total + lax.optimization_barrier(piece).astype(jnp.float32)
        expert_out = lax.optimization_barrier(total.astype(jnp.bfloat16)).astype(jnp.float32)
        weight = jnp.where(live, flat_wts[picks], 0.0)
        return (moe.at[rows].add(weight[:, None] * expert_out), None)
    moe_start = jnp.zeros((row_count, D), jnp.float32)
    numbers = jnp.arange(EXPERTS, dtype=jnp.int32)
    moe, _ = lax.scan(one_expert, moe_start, (w_gate, w_up, w_down, numbers))
    return layer_norm(residual_scale * hidden_one.astype(jnp.float32) + moe, norm2_gain, norm2_bias).astype(jnp.bfloat16)
```

```python
import jax
import jax.numpy as jnp
from jax import lax
from jax.sharding import Mesh
from jax.sharding import PartitionSpec as P

SP = ("sp_0", "sp_1")
GRP_SP = ("grp", "sp_0", "sp_1")
GRP_SP_TP = ("grp", "sp_0", "sp_1", "tp")
SUBLANES = 8

residual_scale = 2.0**0.5
norm_eps = 1e-05


def next_in_sequence(x):
    length = lax.axis_size(SP)
    return lax.ppermute(x, SP, [(i, i + 1) for i in range(length - 1)])


def swapped(x):
    return lax.ppermute(x, "sp_1", [(0, 1), (1, 0)])


def layer_norm(pre, gain, bias):
    center = pre - jnp.mean(pre, axis=-1, keepdims=True)
    spread = jnp.mean(center * center, axis=-1, keepdims=True)
    return center * lax.rsqrt(spread + norm_eps) * gain + bias


def dot(a, b):
    return jnp.dot(a, b, preferred_element_type=jnp.float32)


def chunk_slots(capacity, cores):
    width = SUBLANES // cores
    rest = capacity % width
    sizes = ([rest] if rest else []) + [width] * (capacity // width)
    starts = [sum(sizes[:i]) for i in range(len(sizes))]
    return list(zip(starts, sizes))


def shards(
    gate_in,
    mult_in,
    value_in,
    doc_ids,
    conv_taps,
    out_proj,
    resid,
    norm1_gain,
    norm1_bias,
    expert_ids,
    expert_wts,
    w_gate,
    w_up,
    w_down,
    norm2_gain,
    norm2_bias,
):
    n_tp = lax.axis_size("tp")
    chips = lax.axis_size("sp_0")
    cores = lax.axis_size("sp_1")
    experts = chips * cores
    tok_count, top_count = expert_ids.shape
    width = out_proj.shape[1]
    capacity = 5 * tok_count * top_count // (4 * experts)

    tap_weights = conv_taps.astype(jnp.float32)
    taps = tap_weights.shape[0]
    product = mult_in.astype(jnp.float32) * value_in.astype(jnp.float32)
    docs = doc_ids.astype(jnp.float32)
    row_count, channels = product.shape
    tail_docs = jnp.broadcast_to(docs[row_count - taps + 1 :, None], (taps - 1, channels))
    prev = next_in_sequence(jnp.concatenate([product[row_count - taps + 1 :], tail_docs], axis=0))
    prev_rows, prev_docs = prev[: taps - 1], prev[taps - 1 :, 0]
    meta = jnp.concatenate([expert_ids.astype(jnp.float32).T, expert_wts.T], axis=0)
    metas = jnp.stack([meta, swapped(meta)])

    ext_rows = jnp.concatenate([prev_rows, product], axis=0)
    ext_docs = jnp.concatenate([prev_docs, docs], axis=0)
    filtered = jnp.zeros_like(product)
    for tap_index in range(taps):
        shifted = ext_rows[tap_index : tap_index + row_count]
        same_doc = (ext_docs[tap_index : tap_index + row_count] == docs)[:, None]
        filtered = filtered + tap_weights[tap_index] * jnp.where(same_doc, shifted, 0.0)
    mixed_heads = (gate_in.astype(jnp.float32) * filtered).astype(jnp.bfloat16)
    partial = dot(mixed_heads, out_proj).astype(jnp.bfloat16)
    partials = lax.all_to_all(
        partial.reshape(n_tp, row_count // n_tp, width), "tp", 0, 0, tiled=True
    )
    mixed = jnp.sum(partials.astype(jnp.float32), axis=0)
    hidden_one = layer_norm(
        residual_scale * resid.astype(jnp.float32) + mixed, norm1_gain, norm1_bias
    ).astype(jnp.bfloat16)
    hidden_both = jnp.concatenate([hidden_one, swapped(hidden_one)], axis=0)

    ids, wts = metas[:, :top_count], metas[:, top_count:]
    numbers = (jnp.arange(chips) * cores + lax.axis_index("sp_1")).astype(jnp.float32)
    named = ids[:, :, None, :] == numbers[None, None, :, None]
    chosen = jnp.any(named, axis=1)
    weight = jnp.sum(jnp.where(named, wts[:, :, None, :], 0.0), axis=1)
    before = (jnp.arange(tok_count)[:, None] < jnp.arange(tok_count)[None, :]).astype(jnp.bfloat16)
    earlier = dot(chosen.astype(jnp.bfloat16), before)
    slot_of = jnp.where(chosen, earlier, -1.0)

    def selected(start, size, values):
        slots = (start + jnp.arange(size)).astype(jnp.float32)
        hit = slot_of.transpose(1, 0, 2)[:, :, None, None, :] == slots[None, None, :, None, None]
        same = jnp.arange(cores)[:, None] == jnp.arange(cores)[None, :]
        hit = hit & same[None, :, None, :, None]
        picked = jnp.where(hit, values.transpose(1, 0, 2)[:, :, None, None, :], 0.0)
        return picked.reshape(chips * cores * size, cores * tok_count)

    chunks = chunk_slots(capacity, cores)
    ones = jnp.ones_like(weight)
    packed = [
        dot(selected(start, size, ones).astype(jnp.bfloat16), hidden_both)
        .astype(jnp.bfloat16)
        .reshape(chips, cores * size, width)
        for start, size in chunks
    ]

    gathered = []
    for i in range(len(chunks)):
        moved = lax.all_to_all(packed[i], "sp_0", 0, 0, tiled=True)
        rest = tuple(packed[i + 1 :])
        moved, rest = lax.optimization_barrier((moved, rest))
        packed[i + 1 :] = list(rest)
        gathered.append(lax.all_gather(moved.reshape(-1, width), "tp", axis=0, tiled=True))
    scattered = []
    for rows_in in gathered:
        gate_act = dot(rows_in, w_gate[0])
        up_act = dot(rows_in, w_up[0])
        hid = (jax.nn.silu(gate_act) * up_act).astype(jnp.bfloat16)
        piece = dot(hid, w_down[0]).astype(jnp.bfloat16)
        scattered.append(lax.psum_scatter(piece, "tp", scatter_dimension=0, tiled=True))
    total = jnp.zeros((cores * tok_count, width), jnp.float32)
    for i, (start, size) in enumerate(chunks):
        ready = scattered[i].reshape(chips, cores * size, width)
        back = lax.all_to_all(ready, "sp_0", 0, 0, tiled=True).reshape(-1, width)
        factor = selected(start, size, weight)
        high = factor.astype(jnp.bfloat16)
        low = (factor - high.astype(jnp.float32)).astype(jnp.bfloat16)
        total = total + dot(high.T, back) + dot(low.T, back)
    moe = total[:tok_count] + swapped(total[tok_count:])
    return layer_norm(
        residual_scale * hidden_one.astype(jnp.float32) + moe, norm2_gain, norm2_bias
    ).astype(jnp.bfloat16)


def solution(mesh):
    torus = Mesh(
        mesh.devices.reshape(mesh.shape["grp"], -1, 2, mesh.shape["tp"]),
        ("grp", "sp_0", "sp_1", "tp"),
    )
    in_specs = (
        P(GRP_SP, "tp"),
        P(GRP_SP, "tp"),
        P(GRP_SP, "tp"),
        P(GRP_SP),
        P(None, "tp"),
        P("tp", None),
        P(GRP_SP_TP, None),
        P(),
        P(),
        P(GRP_SP_TP, None),
        P(GRP_SP_TP, None),
        P(SP, None, "tp"),
        P(SP, None, "tp"),
        P(SP, "tp", None),
        P(),
        P(),
    )
    out_specs = P(GRP_SP_TP, None)
    return jax.shard_map(
        shards, mesh=torus, in_specs=in_specs, out_specs=out_specs, check_vma=False
    )
```

```python
import functools

import jax
import jax.numpy as jnp
import numpy as np
from jax import lax
from jax.experimental import pallas as pl
from jax.experimental.pallas import tpu as pltpu
from jax.sharding import Mesh
from jax.sharding import PartitionSpec as P

SP = ("sp_0", "sp_1")
GRP_SP = ("grp", "sp_0", "sp_1")
GRP_SP_TP = ("grp", "sp_0", "sp_1", "tp")
ROWS = 8
HALVES = 2

residual_scale = 2.0**0.5
norm_eps = 1e-05


def next_in_sequence(x):
    length = lax.axis_size(SP)
    return lax.ppermute(x, SP, [(i, i + 1) for i in range(length - 1)])


def turned(x, axis, by):
    length = lax.axis_size(axis)
    return lax.ppermute(x, axis, [(i, (i + by) % length) for i in range(length)])


def swapped(x):
    return turned(x, "sp_1", 1)


def layer_norm(pre, gain, bias):
    center = pre - jnp.mean(pre, axis=-1, keepdims=True)
    spread = jnp.mean(center * center, axis=-1, keepdims=True)
    return center * lax.rsqrt(spread + norm_eps) * gain + bias


def dot(a, b):
    return jnp.dot(a, b, preferred_element_type=jnp.float32)


def local_call(kernel, outs, *args, flops=0):
    return pl.pallas_call(
        kernel,
        out_shape=outs,
        in_specs=[pl.BlockSpec(memory_space=pltpu.VMEM) for _ in args],
        out_specs=jax.tree.map(lambda _: pl.BlockSpec(memory_space=pltpu.VMEM), outs),
        cost_estimate=pl.CostEstimate(flops=flops, bytes_accessed=0, transcendentals=0),
    )(*args)


def block_table(capacity, cores):
    main = capacity // ROWS * ROWS
    rows = []
    for lo, hi in ((0, main), (main, capacity)):
        for half in range(HALVES):
            for core in range(cores):
                rows += [(half, core, slot) for slot in range(lo, hi)]
    return np.array(rows, np.int32)


def pack_kernel(cores, meta_ref, table_ref, own_ref, other_ref, *out_refs):
    tok = own_ref.shape[0]
    half_width = own_ref.shape[1] // HALVES
    expert = table_ref[:, 0:1]
    slot = table_ref[:, 1:2]
    place = table_ref[:, 2:3]
    before = (
        lax.broadcasted_iota(jnp.int32, (tok, tok), 0)
        < lax.broadcasted_iota(jnp.int32, (tok, tok), 1)
    ).astype(jnp.float32).astype(jnp.bfloat16)
    hits = []
    for core in range(cores):
        ids = meta_ref[core]
        named = (ids[0:1, :] == expert) | (ids[1:2, :] == expert)
        named = jnp.where(named, 1.0, 0.0)
        earlier = dot(named.astype(jnp.bfloat16), before)
        hits.append(jnp.where(earlier == slot, named, 0.0))
    total = None
    for half in range(HALVES):
        for core, source in enumerate((own_ref, other_ref)):
            pick = jnp.where(place == float(half * cores + core), hits[core], 0.0)
            rows = source[:, half * half_width : (half + 1) * half_width]
            part = dot(pick.astype(jnp.bfloat16), rows)
            total = part if total is None else total + part
    total = total.astype(jnp.bfloat16)
    size = out_refs[0].shape[0]
    for i, out in enumerate(out_refs):
        out[...] = total[i * size : (i + 1) * size]


def join_kernel(main, *refs):
    blocks, out = refs[:-1], refs[-1]
    count = len(blocks)
    rest = blocks[0].shape[0] - HALVES * main
    for half in range(HALVES):
        for i, block in enumerate(blocks):
            out[(half * count + i) * main : (half * count + i + 1) * main] = block[
                half * main : (half + 1) * main
            ]
    base = HALVES * count * main
    for i, block in enumerate(blocks):
        out[base + i * rest : base + (i + 1) * rest] = block[HALVES * main :]


def spread_kernel(main, count, *refs):
    parts, outs = refs[:-count], refs[-count:]
    total = parts[0][...].astype(jnp.float32)
    for part in parts[1:]:
        total = total + part[...].astype(jnp.float32)
    total = total.astype(jnp.bfloat16)
    rest = outs[0].shape[0] - HALVES * main
    base = HALVES * count * main
    for i, out in enumerate(outs):
        for half in range(HALVES):
            out[half * main : (half + 1) * main] = total[
                (half * count + i) * main : (half * count + i + 1) * main
            ]
        out[HALVES * main :] = total[base + i * rest : base + (i + 1) * rest]


def expert_kernel(main_rows, rest_size, *refs):
    sources = (len(refs) - 5) // 2
    ins, (gate_ref, up_ref, down_ref) = refs[:sources], refs[sources : sources + 3]
    outs = refs[sources + 3 : 2 * sources + 3]
    rows_ref, rest_ref = refs[2 * sources + 3 :]
    half_width = ins[0].shape[1]
    rest_rows = ins[0].shape[0] - HALVES * main_rows
    base = sources * main_rows
    for i, source in enumerate(ins):
        for half in range(HALVES):
            rows_ref[
                i * main_rows : (i + 1) * main_rows, half * half_width : (half + 1) * half_width
            ] = source[half * main_rows : (half + 1) * main_rows]
        rest_ref[i * rest_rows : (i + 1) * rest_rows] = source[HALVES * main_rows :]
    count = sources * rest_rows // HALVES
    shape = (count, HALVES * count)
    row = lax.broadcasted_iota(jnp.int32, shape, 0)
    col = lax.broadcasted_iota(jnp.int32, shape, 1)
    first = (row & ~(rest_size - 1)) * HALVES + (row & (rest_size - 1))
    shape_t = (HALVES * count, count)
    row_t = lax.broadcasted_iota(jnp.int32, shape_t, 0)
    col_t = lax.broadcasted_iota(jnp.int32, shape_t, 1)
    first_t = (col_t & ~(rest_size - 1)) * HALVES + (col_t & (rest_size - 1))
    for half in range(HALVES):
        pick = jnp.where(col == first + half * rest_size, 1.0, 0.0).astype(jnp.bfloat16)
        rows_ref[base : base + count, half * half_width : (half + 1) * half_width] = dot(
            pick, rest_ref[...]
        ).astype(jnp.bfloat16)
    rows = rows_ref[...]
    gate_act = dot(rows, gate_ref[...])
    up_act = dot(rows, up_ref[...])
    hid = (gate_act * jax.nn.sigmoid(gate_act) * up_act).astype(jnp.bfloat16)
    rows_ref[...] = dot(hid, down_ref[...]).astype(jnp.bfloat16)
    rest = None
    for half in range(HALVES):
        pick = jnp.where(row_t == first_t + half * rest_size, 1.0, 0.0).astype(jnp.bfloat16)
        part = dot(
            pick, rows_ref[base : base + count, half * half_width : (half + 1) * half_width]
        )
        rest = part if rest is None else rest + part
    rest_ref[...] = rest.astype(jnp.bfloat16)
    for i, out in enumerate(outs):
        for half in range(HALVES):
            out[half * main_rows : (half + 1) * main_rows] = rows_ref[
                i * main_rows : (i + 1) * main_rows, half * half_width : (half + 1) * half_width
            ]
        out[HALVES * main_rows :] = rest_ref[i * rest_rows : (i + 1) * rest_rows]


def combine_kernel(cores, count, meta_ref, table_ref, *refs):
    blocks, (own_ref, other_ref, all_ref) = refs[:count], refs[count:]
    size = blocks[0].shape[0]
    for i, block in enumerate(blocks):
        all_ref[i * size : (i + 1) * size] = block[...].astype(jnp.float32)
    rows = all_ref[...].astype(jnp.bfloat16)
    tok = own_ref.shape[0]
    half_width = blocks[0].shape[1]
    expert = table_ref[0:1, :]
    slot = table_ref[1:2, :]
    place = table_ref[2:3, :]
    before = (
        lax.broadcasted_iota(jnp.int32, (tok, tok), 1)
        < lax.broadcasted_iota(jnp.int32, (tok, tok), 0)
    ).astype(jnp.float32).astype(jnp.bfloat16)
    for core, out in enumerate((own_ref, other_ref)):
        meta = meta_ref[core]
        first = jnp.where(meta[:, 0:1] == expert, 1.0, 0.0)
        second = jnp.where(meta[:, 1:2] == expert, 1.0, 0.0)
        earlier = dot(before, (first + second).astype(jnp.bfloat16))
        weight = first * meta[:, 2:3] + second * meta[:, 3:4]
        weight = jnp.where(earlier == slot, weight, 0.0)
        high = weight.astype(jnp.bfloat16)
        low = weight - high.astype(jnp.float32)
        high = high.astype(jnp.float32)
        for half in range(HALVES):
            here = place == float(half * cores + core)
            out[:, half * half_width : (half + 1) * half_width] = dot(
                jnp.where(here, high, 0.0).astype(jnp.bfloat16), rows
            ) + dot(jnp.where(here, low, 0.0).astype(jnp.bfloat16), rows)


def distance_groups(length):
    order = [0]
    for step in range(1, length // 2):
        order += [step, length - step]
    order += [length // 2]
    sizes = [6, 6, 4] if length == 16 else [length]
    starts = [sum(sizes[:i]) for i in range(len(sizes))]
    return [order[start : start + size] for start, size in zip(starts, sizes)]


def shards(
    gate_in,
    mult_in,
    value_in,
    doc_ids,
    conv_taps,
    out_proj,
    resid,
    norm1_gain,
    norm1_bias,
    expert_ids,
    expert_wts,
    w_gate,
    w_up,
    w_down,
    norm2_gain,
    norm2_bias,
):
    n_tp = lax.axis_size("tp")
    chips = lax.axis_size("sp_0")
    cores = lax.axis_size("sp_1")
    experts = chips * cores
    tok_count, top_count = expert_ids.shape
    width = out_proj.shape[1]
    half_width = width // HALVES
    capacity = 5 * tok_count * top_count // (4 * experts)
    bf16 = functools.partial(jax.ShapeDtypeStruct, dtype=jnp.bfloat16)
    f32 = functools.partial(jax.ShapeDtypeStruct, dtype=jnp.float32)

    tap_weights = conv_taps.astype(jnp.float32)
    taps = tap_weights.shape[0]
    product = mult_in.astype(jnp.float32) * value_in.astype(jnp.float32)
    docs = doc_ids.astype(jnp.float32)
    row_count, channels = product.shape
    tail_docs = jnp.broadcast_to(docs[row_count - taps + 1 :, None], (taps - 1, channels))
    prev = next_in_sequence(jnp.concatenate([product[row_count - taps + 1 :], tail_docs], axis=0))
    prev_rows, prev_docs = prev[: taps - 1], prev[taps - 1 :, 0]
    meta = jnp.concatenate([expert_ids.astype(jnp.float32).T, expert_wts.T], axis=0)
    metas = jnp.stack([meta, swapped(meta)])

    ext_rows = jnp.concatenate([prev_rows, product], axis=0)
    ext_docs = jnp.concatenate([prev_docs, docs], axis=0)
    filtered = jnp.zeros_like(product)
    for tap_index in range(taps):
        shifted = ext_rows[tap_index : tap_index + row_count]
        same_doc = (ext_docs[tap_index : tap_index + row_count] == docs)[:, None]
        filtered = filtered + tap_weights[tap_index] * jnp.where(same_doc, shifted, 0.0)
    mixed_heads = (gate_in.astype(jnp.float32) * filtered).astype(jnp.bfloat16)

    me = lax.axis_index("tp")
    turns = [n_tp // 2] + [by for by in range(1, n_tp) if by != n_tp // 2]

    def rows_for(by):
        start = (me + by) % n_tp * tok_count
        return dot(lax.dynamic_slice_in_dim(mixed_heads, start, tok_count, 0), out_proj)

    mixed = sum(
        [turned(rows_for(by).astype(jnp.bfloat16), "tp", by).astype(jnp.float32) for by in turns],
        rows_for(0),
    )
    hidden_one = layer_norm(
        residual_scale * resid.astype(jnp.float32) + mixed, norm1_gain, norm1_bias
    ).astype(jnp.bfloat16)
    hidden_other = swapped(hidden_one)

    rows = block_table(capacity, cores)
    main = capacity // ROWS * ROWS * cores
    size = len(rows)
    chip_of = (lax.axis_index("sp_0") + jnp.arange(chips)) % chips
    number = chip_of * cores + lax.axis_index("sp_1")
    table = jnp.stack(
        [
            jnp.repeat(number, size).astype(jnp.float32),
            jnp.asarray(np.tile(rows[:, 2], chips), jnp.float32),
            jnp.asarray(np.tile(rows[:, 0] * cores + rows[:, 1], chips), jnp.float32),
            jnp.zeros((chips * size,), jnp.float32),
        ]
    )
    blocks = local_call(
        functools.partial(pack_kernel, cores),
        [bf16((size, half_width))] * chips,
        metas,
        table.T,
        hidden_one,
        hidden_other,
        flops=2 * chips * size * tok_count * cores * width,
    )

    groups = distance_groups(chips)
    arrived = [[turned(blocks[by], "sp_0", by) if by else blocks[by] for by in g] for g in groups]
    rest_size = (size - HALVES * main) // HALVES
    returned = [None] * chips
    for g, parts in zip(groups, arrived):
        count = len(g)
        joined = local_call(
            functools.partial(join_kernel, main), bf16((count * size, half_width)), *parts
        )
        ins = [joined] + [turned(joined, "tp", by) for by in turns]
        total_rows = n_tp * count * size // HALVES
        outs = pl.pallas_call(
            functools.partial(expert_kernel, count * main, rest_size),
            out_shape=[bf16(joined.shape)] * n_tp,
            in_specs=[pl.BlockSpec(memory_space=pltpu.VMEM)] * (n_tp + 3),
            out_specs=[pl.BlockSpec(memory_space=pltpu.VMEM)] * n_tp,
            scratch_shapes=[
                pltpu.VMEM((total_rows, width), jnp.bfloat16),
                pltpu.VMEM((n_tp * count * rest_size * HALVES, half_width), jnp.bfloat16),
            ],
            cost_estimate=pl.CostEstimate(
                flops=6 * total_rows * width * w_gate.shape[2], bytes_accessed=0, transcendentals=0
            ),
        )(*ins, w_gate[0], w_up[0], w_down[0])
        sums = [outs[0]] + [turned(out, "tp", -by) for out, by in zip(outs[1:], turns)]
        done = local_call(
            functools.partial(spread_kernel, main, count), [bf16((size, half_width))] * count, *sums
        )
        for by, block in zip(g, done):
            returned[by] = turned(block, "sp_0", -by) if by else block
    own, other = pl.pallas_call(
        functools.partial(combine_kernel, cores, chips),
        out_shape=[f32((tok_count, width))] * cores,
        in_specs=[pl.BlockSpec(memory_space=pltpu.VMEM)] * (chips + 2),
        out_specs=[pl.BlockSpec(memory_space=pltpu.VMEM)] * cores,
        scratch_shapes=[pltpu.VMEM((chips * size, half_width), jnp.float32)],
    )(metas.transpose(0, 2, 1), table, *returned)
    moe = own + swapped(other)
    return layer_norm(
        residual_scale * hidden_one.astype(jnp.float32) + moe, norm2_gain, norm2_bias
    ).astype(jnp.bfloat16)


def solution(mesh):
    torus = Mesh(
        mesh.devices.reshape(mesh.shape["grp"], -1, 2, mesh.shape["tp"]),
        ("grp", "sp_0", "sp_1", "tp"),
    )
    in_specs = (
        P(GRP_SP, "tp"),
        P(GRP_SP, "tp"),
        P(GRP_SP, "tp"),
        P(GRP_SP),
        P(None, "tp"),
        P("tp", None),
        P(GRP_SP_TP, None),
        P(),
        P(),
        P(GRP_SP_TP, None),
        P(GRP_SP_TP, None),
        P(SP, None, "tp"),
        P(SP, None, "tp"),
        P(SP, "tp", None),
        P(),
        P(),
    )
    out_specs = P(GRP_SP_TP, None)
    return jax.shard_map(
        shards, mesh=torus, in_specs=in_specs, out_specs=out_specs, check_vma=False
    )
```

```python
import functools

import jax
import jax.numpy as jnp
import numpy as np
from jax import lax
from jax.experimental import pallas as pl
from jax.experimental.pallas import tpu as pltpu
from jax.sharding import Mesh
from jax.sharding import PartitionSpec as P

SP = ("sp_0", "sp_1")
GRP_SP = ("grp", "sp_0", "sp_1")
GRP_SP_TP = ("grp", "sp_0", "sp_1", "tp")
ROWS = 8
HALVES = 2
COLUMNS = 256

residual_scale = 2.0**0.5
norm_eps = 1e-05


def next_in_sequence(x):
    length = lax.axis_size(SP)
    return lax.ppermute(x, SP, [(i, i + 1) for i in range(length - 1)])


def turned(x, axis, by):
    length = lax.axis_size(axis)
    return lax.ppermute(x, axis, [(i, (i + by) % length) for i in range(length)])


def swapped(x):
    return turned(x, "sp_1", 1)


def layer_norm(pre, gain, bias):
    center = pre - jnp.mean(pre, axis=-1, keepdims=True)
    spread = jnp.mean(center * center, axis=-1, keepdims=True)
    return center * lax.rsqrt(spread + norm_eps) * gain + bias


def dot(a, b):
    return jnp.dot(a, b, preferred_element_type=jnp.float32)


def block_table(capacity, cores):
    main = capacity // ROWS * ROWS
    rows = []
    for lo, hi in ((0, main), (main, capacity)):
        for half in range(HALVES):
            for core in range(cores):
                rows += [(half, core, slot) for slot in range(lo, hi)]
    return np.array(rows, np.int32)


def columns(n):
    return pl.ds(pl.multiple_of(n * COLUMNS, COLUMNS), COLUMNS)


def pack_kernel(cores, count, meta_ref, table_ref, own_ref, other_ref, *refs):
    out_refs, (pick_ref, rows_ref, all_ref) = refs[:count], refs[count:]
    tok = own_ref.shape[0]
    half_width = own_ref.shape[1] // HALVES
    expert = table_ref[:, 0:1]
    slot = table_ref[:, 1:2]
    place = table_ref[:, 2:3]
    before = (
        lax.broadcasted_iota(jnp.int32, (tok, tok), 0)
        < lax.broadcasted_iota(jnp.int32, (tok, tok), 1)
    ).astype(jnp.float32).astype(jnp.bfloat16)
    for core, source in enumerate((own_ref, other_ref)):
        ids = meta_ref[core]
        named = (ids[0:1, :] == expert) | (ids[1:2, :] == expert)
        named = jnp.where(named, 1.0, 0.0)
        earlier = dot(named.astype(jnp.bfloat16), before)
        hit = jnp.where(earlier == slot, named, 0.0)
        for half in range(HALVES):
            which = half * cores + core
            pick_ref[:, which * tok : (which + 1) * tok] = jnp.where(
                place == float(which), hit, 0.0
            ).astype(jnp.bfloat16)
            rows_ref[which * tok : (which + 1) * tok] = source[
                :, half * half_width : (half + 1) * half_width
            ]

    def step(n, carry):
        all_ref[:, columns(n)] = dot(pick_ref[...], rows_ref[:, columns(n)]).astype(jnp.bfloat16)
        return carry

    lax.fori_loop(0, half_width // COLUMNS, step, 0)
    size = out_refs[0].shape[0]
    for i, out in enumerate(out_refs):
        out[...] = all_ref[i * size : (i + 1) * size]


def join_kernel(main, count, *refs):
    blocks, out = refs[:count], refs[-1]
    rest = blocks[0].shape[0] - HALVES * main
    for half in range(HALVES):
        for i, block in enumerate(blocks):
            out[(half * count + i) * main : (half * count + i + 1) * main] = block[
                half * main : (half + 1) * main
            ]
    base = HALVES * count * main
    for i, block in enumerate(blocks):
        out[base + i * rest : base + (i + 1) * rest] = block[HALVES * main :]


def spread_kernel(main, count, sources, *refs):
    parts, outs = refs[:sources], refs[-count:]
    total = parts[0][...].astype(jnp.float32)
    for part in parts[1:]:
        total = total + part[...].astype(jnp.float32)
    total = total.astype(jnp.bfloat16)
    rest = outs[0].shape[0] - HALVES * main
    base = HALVES * count * main
    for i, out in enumerate(outs):
        for half in range(HALVES):
            out[half * main : (half + 1) * main] = total[
                (half * count + i) * main : (half * count + i + 1) * main
            ]
        out[HALVES * main :] = total[base + i * rest : base + (i + 1) * rest]


def expert_kernel(main_rows, rest_size, sources, passed, *refs):
    ins, (gate_hbm, up_hbm, down_hbm) = refs[:sources], refs[sources : sources + 3]
    outs = refs[sources + 3 + passed :][:sources]
    rows_ref, rest_ref, hid_ref, gate_ref, up_ref, down_ref, gate_sem, up_sem, down_sem = refs[-9:]
    half_width = ins[0].shape[1]
    rest_rows = ins[0].shape[0] - HALVES * main_rows
    base = sources * main_rows
    hidden_steps = gate_ref.shape[1] // COLUMNS

    def gate_copy(n):
        return pltpu.make_async_copy(
            gate_hbm.at[:, columns(n)], gate_ref.at[:, columns(n)], gate_sem.at[n]
        )

    def up_copy(n):
        return pltpu.make_async_copy(
            up_hbm.at[:, columns(n)], up_ref.at[:, columns(n)], up_sem.at[n]
        )

    down_copy = pltpu.make_async_copy(down_hbm, down_ref, down_sem)
    for n in range(hidden_steps):
        gate_copy(n).start()
        up_copy(n).start()
    down_copy.start()
    for i, source in enumerate(ins):
        for half in range(HALVES):
            rows_ref[
                i * main_rows : (i + 1) * main_rows, half * half_width : (half + 1) * half_width
            ] = source[half * main_rows : (half + 1) * main_rows]
        rest_ref[i * rest_rows : (i + 1) * rest_rows] = source[HALVES * main_rows :]
    count = sources * rest_rows // HALVES
    shape = (count, HALVES * count)
    row = lax.broadcasted_iota(jnp.int32, shape, 0)
    col = lax.broadcasted_iota(jnp.int32, shape, 1)
    first = (row & ~(rest_size - 1)) * HALVES + (row & (rest_size - 1))
    shape_t = (HALVES * count, count)
    row_t = lax.broadcasted_iota(jnp.int32, shape_t, 0)
    col_t = lax.broadcasted_iota(jnp.int32, shape_t, 1)
    first_t = (col_t & ~(rest_size - 1)) * HALVES + (col_t & (rest_size - 1))
    for half in range(HALVES):
        pick = jnp.where(col == first + half * rest_size, 1.0, 0.0).astype(jnp.bfloat16)
        rows_ref[base : base + count, half * half_width : (half + 1) * half_width] = dot(
            pick, rest_ref[...]
        ).astype(jnp.bfloat16)

    def hidden_step(n, carry):
        gate_copy(n).wait()
        up_copy(n).wait()
        gate_act = dot(rows_ref[...], gate_ref[:, columns(n)])
        up_act = dot(rows_ref[...], up_ref[:, columns(n)])
        hid_ref[:, columns(n)] = (gate_act * jax.nn.sigmoid(gate_act) * up_act).astype(jnp.bfloat16)
        return carry

    lax.fori_loop(0, hidden_steps, hidden_step, 0)
    down_copy.wait()

    def down_step(n, carry):
        rows_ref[:, columns(n)] = dot(hid_ref[...], down_ref[:, columns(n)]).astype(jnp.bfloat16)
        return carry

    lax.fori_loop(0, rows_ref.shape[1] // COLUMNS, down_step, 0)
    rest = None
    for half in range(HALVES):
        pick = jnp.where(row_t == first_t + half * rest_size, 1.0, 0.0).astype(jnp.bfloat16)
        part = dot(
            pick, rows_ref[base : base + count, half * half_width : (half + 1) * half_width]
        )
        rest = part if rest is None else rest + part
    rest_ref[...] = rest.astype(jnp.bfloat16)
    for i, out in enumerate(outs):
        for half in range(HALVES):
            out[half * main_rows : (half + 1) * main_rows] = rows_ref[
                i * main_rows : (i + 1) * main_rows, half * half_width : (half + 1) * half_width
            ]
        out[HALVES * main_rows :] = rest_ref[i * rest_rows : (i + 1) * rest_rows]


def expert_call(ins, passed, order, w_gate, w_up, w_down, main_rows, rest_size):
    sources = len(ins)
    rows = sources * ins[0].shape[0] // HALVES
    width = w_gate.shape[0]
    hidden = w_gate.shape[1]
    vmem, anywhere = pl.BlockSpec(memory_space=pltpu.VMEM), pl.BlockSpec(memory_space=pl.ANY)
    outs = pl.pallas_call(
        functools.partial(expert_kernel, main_rows, rest_size, sources, len(passed) + len(order)),
        out_shape=[jax.ShapeDtypeStruct(x.shape, x.dtype) for x in list(ins) + list(passed)],
        in_specs=[vmem] * sources + [anywhere] * (3 + len(passed) + len(order)),
        out_specs=[vmem] * sources + [anywhere] * len(passed),
        input_output_aliases={sources + 3 + i: sources + i for i in range(len(passed))},
        scratch_shapes=[
            pltpu.VMEM((rows, width), jnp.bfloat16),
            pltpu.VMEM((sources * (ins[0].shape[0] - HALVES * main_rows), width // HALVES), jnp.bfloat16),
            pltpu.VMEM((rows, hidden), jnp.bfloat16),
            pltpu.VMEM((width, hidden), jnp.bfloat16),
            pltpu.VMEM((width, hidden), jnp.bfloat16),
            pltpu.VMEM((hidden, width), jnp.bfloat16),
            pltpu.SemaphoreType.DMA((hidden // COLUMNS,)),
            pltpu.SemaphoreType.DMA((hidden // COLUMNS,)),
            pltpu.SemaphoreType.DMA,
        ],
        cost_estimate=pl.CostEstimate(
            flops=6 * rows * width * hidden, bytes_accessed=0, transcendentals=0
        ),
    )(*ins, w_gate, w_up, w_down, *passed, *order)
    return outs[:sources], outs[sources:]


def combine_kernel(cores, count, meta_ref, table_ref, *refs):
    blocks, (own_ref, other_ref, all_ref, high_ref, low_ref) = refs[:count], refs[count:]
    size = blocks[0].shape[0]
    for i, block in enumerate(blocks):
        all_ref[i * size : (i + 1) * size] = block[...]
    tok = own_ref.shape[0]
    half_width = blocks[0].shape[1]
    expert = table_ref[0:1, :]
    slot = table_ref[1:2, :]
    place = table_ref[2:3, :]
    before = (
        lax.broadcasted_iota(jnp.int32, (tok, tok), 1)
        < lax.broadcasted_iota(jnp.int32, (tok, tok), 0)
    ).astype(jnp.float32).astype(jnp.bfloat16)
    for core in range(cores):
        meta = meta_ref[core]
        first = jnp.where(meta[:, 0:1] == expert, 1.0, 0.0)
        second = jnp.where(meta[:, 1:2] == expert, 1.0, 0.0)
        earlier = dot(before, (first + second).astype(jnp.bfloat16))
        weight = first * meta[:, 2:3] + second * meta[:, 3:4]
        weight = jnp.where(earlier == slot, weight, 0.0)
        high = weight.astype(jnp.bfloat16).astype(jnp.float32)
        low = weight - high
        for half in range(HALVES):
            which = half * cores + core
            here = place == float(which)
            lines = slice(which * tok, (which + 1) * tok)
            high_ref[lines] = jnp.where(here, high, 0.0).astype(jnp.bfloat16)
            low_ref[lines] = jnp.where(here, low, 0.0).astype(jnp.bfloat16)

    def step(n, carry):
        rows = all_ref[:, columns(n)]
        total = dot(high_ref[...], rows) + dot(low_ref[...], rows)
        for half in range(HALVES):
            at = pl.ds(pl.multiple_of(half * half_width + n * COLUMNS, COLUMNS), COLUMNS)
            for core, out in enumerate((own_ref, other_ref)):
                which = half * cores + core
                out[:, at] = total[which * tok : (which + 1) * tok]
        return carry

    lax.fori_loop(0, half_width // COLUMNS, step, 0)


def distance_groups(length):
    half = length // 2
    pairs = [(step, length - step) for step in range(1, half)]
    near, middle, far = pairs[: half - 5], pairs[half - 5 : half - 3], pairs[half - 3 :]
    (lead, back), near = near[-1], near[:-1]
    flat = lambda some: [by for pair in some for by in pair]
    return [[0] + flat(near) + [lead], [half, *flat(far[::-1]), back], flat(middle[::-1])]


def shards(
    gate_in,
    mult_in,
    value_in,
    doc_ids,
    conv_taps,
    out_proj,
    resid,
    norm1_gain,
    norm1_bias,
    expert_ids,
    expert_wts,
    w_gate,
    w_up,
    w_down,
    norm2_gain,
    norm2_bias,
):
    n_tp = lax.axis_size("tp")
    chips = lax.axis_size("sp_0")
    cores = lax.axis_size("sp_1")
    experts = chips * cores
    tok_count, top_count = expert_ids.shape
    width = out_proj.shape[1]
    half_width = width // HALVES
    capacity = 5 * tok_count * top_count // (4 * experts)
    bf16 = functools.partial(jax.ShapeDtypeStruct, dtype=jnp.bfloat16)
    f32 = functools.partial(jax.ShapeDtypeStruct, dtype=jnp.float32)

    tap_weights = conv_taps.astype(jnp.float32)
    taps = tap_weights.shape[0]
    product = mult_in.astype(jnp.float32) * value_in.astype(jnp.float32)
    docs = doc_ids.astype(jnp.float32)
    row_count, channels = product.shape
    tail_docs = jnp.broadcast_to(docs[row_count - taps + 1 :, None], (taps - 1, channels))
    prev = next_in_sequence(jnp.concatenate([product[row_count - taps + 1 :], tail_docs], axis=0))
    prev_rows, prev_docs = prev[: taps - 1], prev[taps - 1 :, 0]
    meta = jnp.concatenate([expert_ids.astype(jnp.float32).T, expert_wts.T], axis=0)
    metas = jnp.stack([meta, swapped(meta)])

    ext_rows = jnp.concatenate([prev_rows, product], axis=0)
    ext_docs = jnp.concatenate([prev_docs, docs], axis=0)
    filtered = jnp.zeros_like(product)
    for tap_index in range(taps):
        shifted = ext_rows[tap_index : tap_index + row_count]
        same_doc = (ext_docs[tap_index : tap_index + row_count] == docs)[:, None]
        filtered = filtered + tap_weights[tap_index] * jnp.where(same_doc, shifted, 0.0)
    mixed_heads = (gate_in.astype(jnp.float32) * filtered).astype(jnp.bfloat16)

    me = lax.axis_index("tp")
    turns = [n_tp // 2] + [by for by in range(1, n_tp) if by != n_tp // 2]

    def rows_for(by):
        start = (me + by) % n_tp * tok_count
        return dot(lax.dynamic_slice_in_dim(mixed_heads, start, tok_count, 0), out_proj)

    mixed = sum(
        [turned(rows_for(by).astype(jnp.bfloat16), "tp", by).astype(jnp.float32) for by in turns],
        rows_for(0),
    )
    hidden_one = layer_norm(
        residual_scale * resid.astype(jnp.float32) + mixed, norm1_gain, norm1_bias
    ).astype(jnp.bfloat16)
    hidden_other = swapped(hidden_one)

    rows = block_table(capacity, cores)
    main = capacity // ROWS * ROWS * cores
    size = len(rows)
    chip_of = (lax.axis_index("sp_0") + jnp.arange(chips)) % chips
    number = chip_of * cores + lax.axis_index("sp_1")
    table = jnp.stack(
        [
            jnp.repeat(number, size).astype(jnp.float32),
            jnp.asarray(np.tile(rows[:, 2], chips), jnp.float32),
            jnp.asarray(np.tile(rows[:, 0] * cores + rows[:, 1], chips), jnp.float32),
            jnp.zeros((chips * size,), jnp.float32),
        ]
    )
    packed = pl.pallas_call(
        functools.partial(pack_kernel, cores, chips),
        out_shape=[bf16((size, half_width))] * chips,
        in_specs=[pl.BlockSpec(memory_space=pltpu.VMEM)] * 4,
        out_specs=[pl.BlockSpec(memory_space=pltpu.VMEM)] * chips,
        scratch_shapes=[
            pltpu.VMEM((chips * size, HALVES * cores * tok_count), jnp.bfloat16),
            pltpu.VMEM((HALVES * cores * tok_count, half_width), jnp.bfloat16),
            pltpu.VMEM((chips * size, half_width), jnp.bfloat16),
        ],
    )(metas, table.T, hidden_one, hidden_other)

    blocks = list(packed)
    groups = distance_groups(chips)
    rest_size = (size - HALVES * main) // HALVES
    weights = (w_gate[0], w_up[0], w_down[0])
    returned = [None] * chips
    sums = []

    def gathered(group, order):
        parts = [turned(blocks[by], "sp_0", by) if by else blocks[by] for by in group]
        joined = pl.pallas_call(
            functools.partial(join_kernel, main, len(group)),
            out_shape=bf16((len(group) * size, half_width)),
            in_specs=[pl.BlockSpec(memory_space=pltpu.VMEM)] * len(group)
            + [pl.BlockSpec(memory_space=pl.ANY)] * len(order),
            out_specs=pl.BlockSpec(memory_space=pltpu.VMEM),
        )(*parts, *order)
        return [joined] + [turned(joined, "tp", by) for by in turns]

    def put_back(i, order):
        count = len(groups[i])
        done = pl.pallas_call(
            functools.partial(spread_kernel, main, count, n_tp),
            out_shape=[bf16((size, half_width))] * count,
            in_specs=[pl.BlockSpec(memory_space=pltpu.VMEM)] * n_tp
            + [pl.BlockSpec(memory_space=pl.ANY)] * len(order),
            out_specs=[pl.BlockSpec(memory_space=pltpu.VMEM)] * count,
        )(*sums[i], *order)
        for by, block in zip(groups[i], done):
            returned[by] = turned(block, "sp_0", -by) if by else block
        return done[0]

    def experts_on(i, ins, passed, order):
        outs, passed = expert_call(ins, passed, order, *weights, len(groups[i]) * main, rest_size)
        sums.append([outs[0]] + [turned(out, "tp", -by) for out, by in zip(outs[1:], turns)])
        return passed

    near, far, middle = groups
    held = experts_on(0, gathered(near, []), [blocks[by] for by in middle], [])
    for by, block in zip(middle, held):
        blocks[by] = block
    rows_far = gathered(far, sums[0][:1])
    rows_middle = gathered(middle, [])
    order = [put_back(0, [])]
    experts_on(1, rows_far, [], order)
    experts_on(2, rows_middle, [], [])
    order = [put_back(1, order)]
    put_back(2, order)
    own, other = pl.pallas_call(
        functools.partial(combine_kernel, cores, chips),
        out_shape=[f32((tok_count, width))] * cores,
        in_specs=[pl.BlockSpec(memory_space=pltpu.VMEM)] * (chips + 2),
        out_specs=[pl.BlockSpec(memory_space=pltpu.VMEM)] * cores,
        scratch_shapes=[
            pltpu.VMEM((chips * size, half_width), jnp.bfloat16),
            pltpu.VMEM((HALVES * cores * tok_count, chips * size), jnp.bfloat16),
            pltpu.VMEM((HALVES * cores * tok_count, chips * size), jnp.bfloat16),
        ],
    )(metas.transpose(0, 2, 1), table, *returned)
    moe = own + swapped(other)
    return layer_norm(
        residual_scale * hidden_one.astype(jnp.float32) + moe, norm2_gain, norm2_bias
    ).astype(jnp.bfloat16)


def solution(mesh):
    torus = Mesh(
        mesh.devices.reshape(mesh.shape["grp"], -1, 2, mesh.shape["tp"]),
        ("grp", "sp_0", "sp_1", "tp"),
    )
    in_specs = (
        P(GRP_SP, "tp"),
        P(GRP_SP, "tp"),
        P(GRP_SP, "tp"),
        P(GRP_SP),
        P(None, "tp"),
        P("tp", None),
        P(GRP_SP_TP, None),
        P(),
        P(),
        P(GRP_SP_TP, None),
        P(GRP_SP_TP, None),
        P(SP, None, "tp"),
        P(SP, None, "tp"),
        P(SP, "tp", None),
        P(),
        P(),
    )
    out_specs = P(GRP_SP_TP, None)
    return jax.shard_map(
        shards, mesh=torus, in_specs=in_specs, out_specs=out_specs, check_vma=False
    )
```
